32 devices in a mesh: ep: 8 (over z, x), tp: 4 (over y, core).
Axes of the slice: x: 2, y: 2, z: 4, core: 2. Of those that a mesh axis runs over, the one named last changes fastest.
Arguments:
- mixer_input: bfloat16 [2048, 2048], P('ep', 'tp'), may hold values from -80 to 80
- mixer_gain: float32 [2048], P('tp'), may hold values from 0.1 to 1.9
- time_step: float32 [2048, 128], P('ep', 'tp'), may hold values from 0.25 to 4
- pole_real: float32 [128, 32], P('tp'), may hold values from -0.1 to 0, as said below
- pole_imag: float32 [128, 32], P('tp'), may hold values from 0.25 to 3
- input_real: float32 [128, 32, 16], P('tp'), may hold values from -1 to 1
- input_imag: float32 [128, 32, 16], P('tp'), may hold values from -1 to 1
- read_real: float32 [128, 16, 32], P('tp'), may hold values from -1 to 1
- read_imag: float32 [128, 16, 32], P('tp'), may hold values from -1 to 1
- out_value: bfloat16 [2048, 2048], P(None, 'tp'), may hold values from -0.125 to 0.125
- out_gate: bfloat16 [2048, 2048], P(None, 'tp'), may hold values from -0.125 to 0.125
- expert_input: bfloat16 [1024, 2048], P('ep', 'tp'), may hold values from -80 to 80
- expert_gain: float32 [2048], P('tp'), may hold values from 0.1 to 1.9
- routes: int32 [1024, 2], P('ep'), may hold values from 0 to 7, all different within a row; in each aligned block of 128 rows (0 to 127, 128 to 255, ...) at most 64 rows name the same one
- route_weight: float32 [1024, 2], P('ep'), may hold values from 0.2 to 1
- expert_gate: bfloat16 [8, 2048, 4096], P('ep', None, 'tp'), may hold values from -0.125 to 0.125
- expert_up: bfloat16 [8, 2048, 4096], P('ep', None, 'tp'), may hold values from -0.125 to 0.125
- expert_down: bfloat16 [8, 4096, 2048], P('ep', 'tp'), may hold values from -0.125 to 0.125
Outputs:
- mixer_output: bfloat16 [2048, 2048], P('ep', 'tp')
- expert_output: bfloat16 [1024, 2048], P('ep', 'tp')
The draws below stay inside these ranges and needn't reach their ends.
Inputs may be any that keep to these rules, and one draw needn't show every extreme that they name: `routes`: each row names 2 different experts. Among the 128 rows of one index of ep, no expert is named more than 64 times, a bound that some block reaches in some of them. `pole_real`: every rate is negative.
All inputs are finite; a program needn't handle non-finite values.
Results may differ from the reference program's by a relative error of at most 0.02.
Values may be sent and summed in bfloat16 or wider, within the bound.
A program may use at most 128 MiB of HBM per device.

```python
import math
import jax
import jax.numpy as jnp
import numpy as np
from jax import lax

D = 2048
GROUP_CH = 16
GROUPS = 128
STATE = 32
FFE = 4096
EXPERTS = 8
TOP = 2
TOK_A = 256
TOK_B = 128
BLOCK = 128
SEQ_A = 2048
SEQ_B = 1024
CAP = 64
N_EP = 8
N_TP = 4


def scaled_rows(key, length):
    first, second, third = jax.random.split(key, 3)
    base = jnp.clip(jax.random.normal(first, (length, D), jnp.float32), -6.0, 6.0)
    levels = jnp.exp(jax.random.uniform(second, (16,), jnp.float32, -1.1, 1.1))
    column_scale = jnp.repeat(levels, D // 16)
    return base * column_scale[None, :]


def draw_mixer_input(key, part):
    return scaled_rows(jax.random.fold_in(key, 7), SEQ_A).astype(jnp.bfloat16)


def draw_expert_input(key, part):
    return scaled_rows(jax.random.fold_in(key, 8), SEQ_B).astype(jnp.bfloat16)


def draw_time_step(key, part):
    first, second = jax.random.split(jax.random.fold_in(key, 9))
    spans = SEQ_A // TOK_A
    fine = jax.random.uniform(first, (SEQ_A, GROUPS), jnp.float32, -0.5, 0.5)
    coarse = jax.random.uniform(second, (spans, 1, GROUPS), jnp.float32, -0.8, 0.8)
    coarse = jnp.broadcast_to(coarse, (spans, TOK_A, GROUPS)).reshape(SEQ_A, GROUPS)
    return jnp.exp(fine + coarse)


def rate_table(key):
    first, second, third = jax.random.split(jax.random.fold_in(key, 101), 3)
    share = 0.5
    slow = jax.random.uniform(first, (GROUPS, STATE), jnp.float32) < share
    slow_rate = jnp.exp(jax.random.uniform(second, (GROUPS, STATE), jnp.float32, math.log(0.1), math.log(0.6))) / SEQ_A
    fast_rate = jnp.exp(jax.random.uniform(third, (GROUPS, STATE), jnp.float32, math.log(0.03), math.log(0.1)))
    return jnp.where(slow, slow_rate, fast_rate)


def draw_pole_real(key, part):
    return -rate_table(key)


def read_table(key, salt):
    rates = rate_table(key)
    scale = jnp.sqrt(2.4 * rates / STATE) * 1.4
    noise = jnp.clip(jax.random.normal(jax.random.fold_in(key, salt), (GROUPS, GROUP_CH, STATE), jnp.float32), -4.0, 4.0)
    return noise * scale[:, None, :]


def draw_read_real(key, part):
    return read_table(key, 202)


def draw_read_imag(key, part):
    return read_table(key, 203)


def spiked(values, rng, source, target, parts, factor):
    owner, partner = [(jnp.arange(values.shape[dim]) // (values.shape[dim] // parts)).reshape([-1 if axis == dim else 1 for axis in range(values.ndim)]) for dim in (source, target)]
    chosen = jax.random.permutation(rng, parts)[partner]
    strong = (owner == chosen) | (owner == (partner + parts // 2) % parts)
    return jnp.where(strong, factor * values, values)


def block_scale(own_key, dims, cuts, low, top_value):
    level, own = 1.0, jax.random.fold_in(own_key, 6)
    for position, shards_of in cuts:
        steps = jnp.exp(jax.random.uniform(jax.random.fold_in(own, position), (shards_of,), jnp.float32, low / len(cuts), top_value / len(cuts)))
        level = level * jnp.repeat(steps, dims[position] // shards_of).reshape([-1 if axis == position else 1 for axis in range(len(dims))])
    return level


def deal_out(stream_key, own, number, rows, number_of, top, reach, skew):
    ranking = jax.random.permutation(stream_key, number_of)
    heavy_load, common = portions_of(number_of, rows * top, reach, skew, True), portions_of(number_of, rows * top, reach, skew, False)
    places = jnp.arange(number_of)

    def named(sizes, offset_by):
        used = int((sizes > 0).sum())
        fixed = max(1, used // 4)
        moved = fixed + (places - fixed + offset_by * (used - fixed)) % max(1, number_of - fixed)
        return jnp.zeros((number_of,), jnp.int32).at[ranking[jnp.where(places < fixed, places, moved)]].set(jnp.asarray(sizes, jnp.int32))

    sizes = jnp.where(number % 4 == 0, named(heavy_load, number // 4), named(common, number - number // 4 - 1))
    mixed = jax.random.permutation(jax.random.fold_in(own, 3), number_of)
    source_of, taker = mixed[0:number_of // 2 * 2:2], mixed[1:number_of // 2 * 2:2]
    margin = jnp.minimum(sizes[source_of] - 1, reach - sizes[taker]) // 2
    margin = jnp.where((source_of == ranking[0]) | (taker == ranking[0]) | (sizes[taker] == 0), 0, jnp.maximum(margin, 0))
    moved = jax.random.randint(jax.random.fold_in(own, 4), (number_of // 2,), 0, 1 << 20) % (margin + 1)
    sizes = sizes.at[source_of].add(-moved).at[taker].add(moved)
    items = jnp.searchsorted(jnp.cumsum(sizes), jnp.arange(rows * top), side="right").astype(jnp.int32)
    table = items.reshape(top, rows).T
    table = table[jax.random.permutation(jax.random.fold_in(own, 1), rows)]
    offset_by = jax.random.randint(jax.random.fold_in(own, 2), (rows, 1), 0, top)
    return jnp.take_along_axis(table, (jnp.arange(top)[None, :] + offset_by) % top, axis=1)


def portions_of(amount, total, most, slope, full):
    weights = [(1 << 20) // math.isqrt(rank ** slope) + 1 for rank in range(1, amount + 1)]
    largest = most if full else min(most, max(-(-total // amount), total * weights[0] // sum(weights)))
    least = 1 if total - largest >= amount - 1 else 0
    counts, rest = [largest] + [least] * (amount - 1), total - largest - least * (amount - 1)
    while rest > 0:
        movable = [i for i in range(1, amount) if counts[i] < largest] or [i for i in range(1, amount) if counts[i] < most]
        pool, budget = sum([weights[i] for i in movable]), rest
        for i in movable:
            more = min(most - counts[i], max(1, budget * weights[i] // pool), rest)
            counts[i] = counts[i] + more
            rest = rest - more
    return np.array(counts)


def scatter_about(key, shape, width, bound, shards=(), held_as=jnp.bfloat16):
    values = width * jax.random.normal(key, shape, jnp.float32)
    if shards:
        values = values * block_scale(key, shape, shards, -0.22, 0.18)
    return jnp.clip(values, -bound, bound).astype(held_as)


def bell_draw_with(rng, extent, spread, reach, shards, heavy, kind=jnp.bfloat16):
    array = spread * jax.random.normal(rng, extent, jnp.float32)
    if shards:
        array = array * block_scale(rng, extent, shards, -0.22, 0.18)
    return jnp.clip(spiked(array, jax.random.fold_in(rng, 3), *heavy), -reach, reach).astype(kind)


def setup_inputs(seed: int = 0) -> dict:
    keys = jax.random.split(jax.random.key(seed), 19)
    mixer_input = draw_mixer_input(jax.random.fold_in(keys[18], 71), 0)
    mixer_gain = jnp.clip(1.0 + 0.18 * jax.random.normal(keys[1], (D,), jnp.float32), 0.1, 1.9)
    time_step = draw_time_step(jax.random.fold_in(keys[18], 71), 0)
    pole_real = draw_pole_real(jax.random.fold_in(keys[18], 71), 0)
    pole_imag = jnp.clip(0.25 + 2.75 * jax.random.uniform(keys[4], (GROUPS, STATE), jnp.float32) ** block_scale(keys[4], (GROUPS, STATE), ((0, 4),), -0.2, 0.2), 0.25, 3.0)
    input_real = scatter_about(keys[5], (GROUPS, STATE, GROUP_CH), (2 * GROUP_CH) ** -0.5, 1.0, ((0, 4),), jnp.float32)
    input_imag = scatter_about(keys[6], (GROUPS, STATE, GROUP_CH), (2 * GROUP_CH) ** -0.5, 1.0, ((0, 4),), jnp.float32)
    read_real = draw_read_real(jax.random.fold_in(keys[18], 71), 0)
    read_imag = draw_read_imag(jax.random.fold_in(keys[18], 71), 0)
    out_value = scatter_about(keys[9], (D, D), D ** -0.5, 0.125, ((1, 4),))
    out_gate = scatter_about(keys[10], (D, D), D ** -0.5, 0.125, ((1, 4),))
    expert_input = draw_expert_input(jax.random.fold_in(keys[18], 71), 0)
    expert_gain = jnp.clip(1.0 + 0.18 * jax.random.normal(keys[12], (D,), jnp.float32), 0.1, 1.9)
    routes_keys = jax.random.split(jax.random.fold_in(keys[13], 1), SEQ_B // TOK_B)
    routes_turns = jax.random.permutation(jax.random.fold_in(keys[13], 3), SEQ_B // TOK_B)
    routes = jax.vmap(lambda own, number: deal_out(jax.random.fold_in(keys[13], 2), own, number, TOK_B, EXPERTS, TOP, CAP, 1))(routes_keys, routes_turns).reshape((SEQ_B, TOP))
    route_weight = jnp.clip(0.2 + 0.8 * jax.random.uniform(keys[14], (SEQ_B, TOP), jnp.float32) ** block_scale(keys[14], (SEQ_B, TOP), ((0, 8),), -0.2, 0.2), 0.2, 1.0)
    expert_gate = scatter_about(keys[15], (EXPERTS, D, FFE), D ** -0.5, 0.125, ((0, 8), (2, 4)))
    expert_up = scatter_about(keys[16], (EXPERTS, D, FFE), D ** -0.5, 0.125, ((0, 8), (2, 4)))
    expert_down = bell_draw_with(keys[17], (EXPERTS, FFE, D), FFE ** -0.5, 0.125, ((0, 8), (1, 4)), (1, 2, 4, 2.0))
    return dict(mixer_input=mixer_input, mixer_gain=mixer_gain, time_step=time_step, pole_real=pole_real, pole_imag=pole_imag, input_real=input_real, input_imag=input_imag, read_real=read_real, read_imag=read_imag, out_value=out_value, out_gate=out_gate, expert_input=expert_input, expert_gain=expert_gain, routes=routes, route_weight=route_weight, expert_gate=expert_gate, expert_up=expert_up, expert_down=expert_down)


def layer_norm(rows, gain):
    wide = rows.astype(jnp.float32)
    average = lax.optimization_barrier(jnp.mean(wide, axis=1, keepdims=True))
    variance = lax.optimization_barrier(jnp.mean(wide * wide, axis=1, keepdims=True)) - average * average
    return (wide - average) * lax.rsqrt(variance + 1e-05) * gain[None, :]

def compose(earlier, later):
    a1r, a1i, b1r, b1i = earlier
    a2r, a2i, b2r, b2i = later
    return (a2r * a1r - a2i * a1i, a2r * a1i + a2i * a1r, a2r * b1r - a2i * b1i + b2r, a2r * b1i + a2i * b1r + b2i)

def mixer_part(mixer_input, mixer_gain, time_step, pole_real, pole_imag, input_real, input_imag, read_real, read_imag, out_value, out_gate):
    normed = layer_norm(mixer_input, mixer_gain)
    blocks = SEQ_A // BLOCK
    rows_in = normed.reshape(blocks, BLOCK, GROUPS, GROUP_CH)
    steps_in = time_step.reshape(blocks, BLOCK, GROUPS)
    denom = pole_real * pole_real + pole_imag * pole_imag
    highest = lax.Precision.HIGHEST

    def advance(carried, inputs):
        state_re, state_im = carried
        rows_blk, step_blk = inputs
        drive_re = jnp.einsum('tgm,gpm->tgp', rows_blk, input_real, precision=highest)
        drive_im = jnp.einsum('tgm,gpm->tgp', rows_blk, input_imag, precision=highest)
        delta = step_blk[:, :, None]
        magnitude = jnp.exp(pole_real[None] * delta)
        angle = pole_imag[None] * delta
        abar_re = magnitude * jnp.cos(angle)
        abar_im = magnitude * jnp.sin(angle)
        numer_re = abar_re - 1.0
        coef_re = (numer_re * pole_real[None] + abar_im * pole_imag[None]) / denom[None]
        coef_im = (abar_im * pole_real[None] - numer_re * pole_imag[None]) / denom[None]
        push_re = coef_re * drive_re - coef_im * drive_im
        push_im = coef_re * drive_im + coef_im * drive_re
        cum_re, cum_im, acc_re, acc_im = lax.associative_scan(compose, (abar_re, abar_im, push_re, push_im), axis=0)
        new_re = cum_re * state_re[None] - cum_im * state_im[None] + acc_re
        new_im = cum_re * state_im[None] + cum_im * state_re[None] + acc_im
        response = jnp.einsum('gmp,tgp->tgm', read_real, new_re, precision=highest) - jnp.einsum('gmp,tgp->tgm', read_imag, new_im, precision=highest)
        mixed_blk = jax.nn.gelu(response.reshape(BLOCK, D)).astype(jnp.bfloat16)
        return ((new_re[-1], new_im[-1]), mixed_blk)
    zeros_state = jnp.zeros((GROUPS, STATE), jnp.float32)
    unused, mixed = lax.scan(advance, (zeros_state, zeros_state), (rows_in, steps_in))
    mixed = mixed.reshape(SEQ_A, D)
    value_sum = jnp.dot(mixed, out_value, preferred_element_type=jnp.float32)
    gate_sum = jnp.dot(mixed, out_gate, preferred_element_type=jnp.float32)
    return (value_sum * jax.nn.sigmoid(gate_sum)).astype(jnp.bfloat16)

def expert_part(expert_input, expert_gain, routes, route_weight, expert_gate, expert_up, expert_down):
    normed = layer_norm(expert_input, expert_gain).astype(jnp.bfloat16)
    tokens = normed.shape[0]
    flat_routes = routes.reshape(-1)
    flat_weights = route_weight.reshape(-1)
    owners = jnp.arange(flat_routes.shape[0], dtype=jnp.int32) // TOP
    padded = jnp.concatenate([normed, jnp.zeros((1, D), jnp.bfloat16)], axis=0)
    limit = N_EP * CAP
    blocks = FFE // N_TP

    def one_expert(totals, index):
        hits = flat_routes == index
        where_to = jnp.cumsum(hits.astype(jnp.int32)) - 1
        target = jnp.where(hits, where_to, limit).astype(jnp.int32)
        holder = jnp.full((limit,), tokens, jnp.int32).at[target].set(owners, mode='drop')
        share = jnp.zeros((limit,), jnp.float32).at[target].set(flat_weights, mode='drop')
        rows = padded[holder]
        gate_w = lax.dynamic_index_in_dim(expert_gate, index, 0, keepdims=False)
        up_w = lax.dynamic_index_in_dim(expert_up, index, 0, keepdims=False)
        down_w = lax.dynamic_index_in_dim(expert_down, index, 0, keepdims=False)
        gate_val = jnp.dot(rows, gate_w, preferred_element_type=jnp.float32)
        up_val = jnp.dot(rows, up_w, preferred_element_type=jnp.float32)
        hidden = (jax.nn.silu(gate_val) * up_val).astype(jnp.bfloat16)
        pieces = hidden.reshape(limit, N_TP, blocks).astype(jnp.float32)
        down_pieces = down_w.reshape(N_TP, blocks, D).astype(jnp.float32)
        partial_value = jnp.einsum('snk,nkd->nsd', pieces, down_pieces).astype(jnp.bfloat16)
        result = lax.optimization_barrier(jnp.sum(partial_value.astype(jnp.float32), axis=0)).astype(jnp.bfloat16)
        contrib = result.astype(jnp.float32) * share[:, None]
        return (totals.at[holder].add(contrib), None)
    totals, unused = lax.scan(one_expert, jnp.zeros((tokens + 1, D), jnp.float32), jnp.arange(EXPERTS, dtype=jnp.int32))
    return totals[:tokens].astype(jnp.bfloat16)

def reference(mixer_input, mixer_gain, time_step, pole_real, pole_imag, input_real, input_imag, read_real, read_imag, out_value, out_gate, expert_input, expert_gain, routes, route_weight, expert_gate, expert_up, expert_down):
    mixer_output = mixer_part(mixer_input, mixer_gain, time_step, pole_real, pole_imag, input_real, input_imag, read_real, read_imag, out_value, out_gate)
    expert_output = expert_part(expert_input, expert_gain, routes, route_weight, expert_gate, expert_up, expert_down)
    return (mixer_output, expert_output)
```

```python
import functools
import jax
import jax.numpy as jnp
from jax import lax
from jax.experimental import pallas as pl
from jax.experimental.pallas import tpu as pltpu
from jax.sharding import PartitionSpec as P

norm_eps = 1e-05
highest = lax.Precision.HIGHEST
CHUNKS = 8
TILE = 256


def sin_cos(angle):
    turns = jnp.round(angle * 0.6366197723675814)
    left = angle - turns * 1.5703125
    left = left - turns * 4.83751296997e-4
    left = left - turns * 7.549789948768648e-8
    sq = left * left
    sine = ((-1.9515295891e-4 * sq + 8.3321608736e-3) * sq - 1.6666654611e-1) * sq * left + left
    cosine = (
        ((2.443315711809948e-5 * sq - 1.388731625493765e-3) * sq + 4.166664568298827e-2) * sq * sq
        - 0.5 * sq
        + 1.0
    )
    quadrant = turns.astype(jnp.int32)
    odd = (quadrant & 1) == 1
    sin_out = jnp.where(odd, cosine, sine)
    cos_out = jnp.where(odd, sine, cosine)
    sin_out = jnp.where((quadrant & 2) == 2, -sin_out, sin_out)
    cos_out = jnp.where(((quadrant + 1) & 2) == 2, -cos_out, cos_out)
    return sin_out, cos_out


def nt(left, right, **kw):
    return lax.dot_general(
        left, right, (((1,), (1,)), ((), ())), preferred_element_type=jnp.float32, **kw
    )


def spread(table, row_div, lane_div):
    rows, width = table.shape
    lanes = width * (rows // row_div)
    src = lax.broadcasted_iota(jnp.int32, (width, lanes), 0)
    dst = lax.broadcasted_iota(jnp.int32, (width, lanes), 1)
    pick = (src == dst % width).astype(jnp.bfloat16)
    wide = jnp.dot(table.astype(jnp.bfloat16), pick, preferred_element_type=jnp.float32)
    row = lax.broadcasted_iota(jnp.int32, (rows, lanes), 0) // row_div
    lane = lax.broadcasted_iota(jnp.int32, (rows, lanes), 1) // lane_div
    return jnp.where(row == lane, wide, 0.0).astype(jnp.bfloat16)


def mixer_kernel(
    width,
    rows_ref,
    stats_ref,
    gain_ref,
    step_ref,
    pole_ref,
    in_re_ref,
    in_im_ref,
    rd_re_ref,
    rd_im_ref,
    out_ref,
    a_re,
    a_im,
    u_re,
    u_im,
    sums,
    enter,
    mixed_ref,
    mine_ref,
    slots_ref,
    send_sems,
    recv_sems,
):
    count = slots_ref.shape[0]
    me = lax.axis_index("ep")
    barrier = pltpu.get_barrier_semaphore()
    for k in range(1, count):
        pl.semaphore_signal(
            barrier,
            inc=1,
            device_id={"ep": lax.rem(me + k, count)},
            device_id_type=pl.DeviceIdType.MESH,
        )

    positions, channels = rows_ref.shape
    groups = step_ref.shape[1]
    flat = a_re.shape[1]
    states = flat // groups
    group_ch = channels // groups
    tiles = flat // TILE
    per_tile = TILE // states
    tile_ch = per_tile * group_ch
    steps = positions // CHUNKS

    average = stats_ref[:, 0:1] / width
    variance = stats_ref[:, 1:2] / width - average * average
    normed = (rows_ref[...].astype(jnp.float32) - average) * lax.rsqrt(variance + norm_eps)
    normed = (normed * gain_ref[...]).astype(jnp.bfloat16)
    to_row = lax.broadcasted_iota(jnp.int32, (positions, positions), 0)
    from_row = lax.broadcasted_iota(jnp.int32, (positions, positions), 1)
    order = from_row == (to_row % CHUNKS) * steps + to_row // CHUNKS
    order16 = order.astype(jnp.bfloat16)
    normed = jnp.dot(order16, normed, preferred_element_type=jnp.float32).astype(jnp.bfloat16)
    step = jnp.dot(
        order.astype(jnp.float32), step_ref[...], precision=highest,
        preferred_element_type=jnp.float32,
    )

    for tile in range(tiles):
        lanes = slice(tile * TILE, (tile + 1) * TILE)
        source = lax.broadcasted_iota(jnp.int32, (groups, TILE), 0)
        owner = lax.broadcasted_iota(jnp.int32, (groups, TILE), 1) // states + tile * per_tile
        a_re[:, lanes] = jnp.dot(
            step, (source == owner).astype(jnp.float32), precision=highest,
            preferred_element_type=jnp.float32,
        )
        piece = normed[:, tile * tile_ch : (tile + 1) * tile_ch]
        u_re[:, lanes] = nt(piece, spread(in_re_ref[lanes, :], states, group_ch))
        u_im[:, lanes] = nt(piece, spread(in_im_ref[lanes, :], states, group_ch))
        p_re, p_im = pole_ref[0:1, lanes], pole_ref[1:2, lanes]
        d_re, d_im = pole_ref[2:3, lanes], pole_ref[3:4, lanes]

        def first(s, carried, lanes=lanes, p_re=p_re, p_im=p_im, d_re=d_re, d_im=d_im):
            c_re, c_im, s_re, s_im = carried
            here = pl.ds(pl.multiple_of(s * CHUNKS, CHUNKS), CHUNKS)
            delta = a_re[here, lanes]
            magnitude = jnp.exp(p_re * delta)
            sine, cosine = sin_cos(p_im * delta)
            ab_re = magnitude * cosine
            ab_im = magnitude * sine
            numer = ab_re - 1.0
            k_re = numer * d_re + ab_im * d_im
            k_im = ab_im * d_re - numer * d_im
            v_re, v_im = u_re[here, lanes], u_im[here, lanes]
            w_re = k_re * v_re - k_im * v_im
            w_im = k_re * v_im + k_im * v_re
            a_re[here, lanes] = ab_re
            a_im[here, lanes] = ab_im
            u_re[here, lanes] = w_re
            u_im[here, lanes] = w_im
            return (
                ab_re * c_re - ab_im * c_im,
                ab_re * c_im + ab_im * c_re,
                ab_re * s_re - ab_im * s_im + w_re,
                ab_re * s_im + ab_im * s_re + w_im,
            )

        zero = jnp.zeros((CHUNKS, TILE), jnp.float32)
        found = lax.fori_loop(0, steps, first, (zero + 1.0, zero, zero, zero), unroll=4)
        for index, part in enumerate(found):
            sums[index, :, lanes] = part

    def chunk(index, c):
        return sums[index, c : c + 1, :]

    c_re, c_im, s_re, s_im = (chunk(index, 0) for index in range(4))
    for c in range(1, CHUNKS):
        b_re, b_im = chunk(0, c), chunk(1, c)
        c_re, c_im = b_re * c_re - b_im * c_im, b_re * c_im + b_im * c_re
        s_re, s_im = (
            b_re * s_re - b_im * s_im + chunk(2, c),
            b_re * s_im + b_im * s_re + chunk(3, c),
        )
    mine_ref[0:1, :] = c_re
    mine_ref[1:2, :] = c_im
    mine_ref[2:3, :] = s_re
    mine_ref[3:4, :] = s_im

    pl.semaphore_wait(barrier, count - 1)
    copies = []
    for k in range(1, count):
        copy = pltpu.make_async_remote_copy(
            src_ref=mine_ref,
            dst_ref=slots_ref.at[k],
            send_sem=send_sems.at[k],
            recv_sem=recv_sems.at[k],
            device_id={"ep": lax.rem(me + k, count)},
            device_id_type=pl.DeviceIdType.MESH,
        )
        copy.start()
        copies.append(copy)
    read_re = [
        spread(rd_re_ref[t * tile_ch : (t + 1) * tile_ch, :], group_ch, states)
        for t in range(tiles)
    ]
    read_im = [
        spread(rd_im_ref[t * tile_ch : (t + 1) * tile_ch, :], group_ch, states)
        for t in range(tiles)
    ]
    for copy in copies:
        copy.wait()

    def fold(position, carried):
        h_re, h_im = carried
        slot = me - position
        b_re, b_im = slots_ref[slot, 0:1, :], slots_ref[slot, 1:2, :]
        return (
            b_re * h_re - b_im * h_im + slots_ref[slot, 2:3, :],
            b_re * h_im + b_im * h_re + slots_ref[slot, 3:4, :],
        )

    blank = jnp.zeros((1, flat), jnp.float32)
    h_re, h_im = lax.fori_loop(0, me, fold, (blank, blank))
    for c in range(CHUNKS):
        enter[0, c : c + 1, :] = h_re
        enter[1, c : c + 1, :] = h_im
        b_re, b_im = chunk(0, c), chunk(1, c)
        h_re, h_im = (
            b_re * h_re - b_im * h_im + chunk(2, c),
            b_re * h_im + b_im * h_re + chunk(3, c),
        )

    for tile in range(tiles):
        lanes = slice(tile * TILE, (tile + 1) * TILE)

        def second(s, carried, lanes=lanes):
            s_re, s_im = carried
            here = pl.ds(pl.multiple_of(s * CHUNKS, CHUNKS), CHUNKS)
            ab_re, ab_im = a_re[here, lanes], a_im[here, lanes]
            n_re = ab_re * s_re - ab_im * s_im + u_re[here, lanes]
            n_im = ab_re * s_im + ab_im * s_re + u_im[here, lanes]
            u_re[here, lanes] = n_re
            u_im[here, lanes] = n_im
            return n_re, n_im

        lax.fori_loop(0, steps, second, (enter[0, :, lanes], enter[1, :, lanes]), unroll=8)
        response = nt(u_re[:, lanes].astype(jnp.bfloat16), read_re[tile]) - nt(
            u_im[:, lanes].astype(jnp.bfloat16), read_im[tile]
        )
        mixed_ref[:, tile * tile_ch : (tile + 1) * tile_ch] = jax.nn.gelu(response).astype(
            jnp.bfloat16
        )
    back = (to_row == (from_row % CHUNKS) * steps + from_row // CHUNKS).astype(jnp.bfloat16)
    out_ref[...] = jnp.dot(
        back, mixed_ref[...], preferred_element_type=jnp.float32
    ).astype(jnp.bfloat16)


def mix(rows, stats, gain, step, pole, in_re, in_im, rd_re, rd_im, width):
    positions, channels = rows.shape
    flat = pole.shape[1]
    count = lax.axis_size("ep")
    f32 = jnp.float32
    return pl.pallas_call(
        functools.partial(mixer_kernel, width),
        out_shape=jax.ShapeDtypeStruct((positions, channels), jnp.bfloat16),
        in_specs=[pl.BlockSpec(memory_space=pltpu.VMEM)] * 9,
        out_specs=pl.BlockSpec(memory_space=pltpu.VMEM),
        scratch_shapes=[
            pltpu.VMEM((positions, flat), f32),
            pltpu.VMEM((positions, flat), f32),
            pltpu.VMEM((positions, flat), f32),
            pltpu.VMEM((positions, flat), f32),
            pltpu.VMEM((4, CHUNKS, flat), f32),
            pltpu.VMEM((2, CHUNKS, flat), f32),
            pltpu.VMEM((positions, channels), jnp.bfloat16),
            pltpu.VMEM((4, flat), f32),
            pltpu.VMEM((count, 4, flat), f32),
            pltpu.SemaphoreType.DMA((count,)),
            pltpu.SemaphoreType.DMA((count,)),
        ],
        compiler_params=pltpu.CompilerParams(
            collective_id=0, has_side_effects=True, vmem_limit_bytes=24 * 1024 * 1024
        ),
        cost_estimate=pl.CostEstimate(
            flops=2 * positions * flat * 400, bytes_accessed=4 * positions * flat, transcendentals=0
        ),
    )(rows, stats, gain, step, pole, in_re, in_im, rd_re, rd_im)


def row_moments(rows):
    wide = rows.astype(jnp.float32)
    return (jnp.sum(wide, axis=1), jnp.sum(wide * wide, axis=1))


def normalize(rows, sums, squares, gain, width):
    average = sums / width
    variance = squares / width - average * average
    wide = rows.astype(jnp.float32)
    return (wide - average[:, None]) * lax.rsqrt(variance[:, None] + norm_eps) * gain[None, :]


def shards(
    mixer_input,
    mixer_gain,
    time_step,
    pole_real,
    pole_imag,
    input_real,
    input_imag,
    read_real,
    read_imag,
    out_value,
    out_gate,
    expert_input,
    expert_gain,
    routes,
    route_weight,
    expert_gate,
    expert_up,
    expert_down,
):
    width = mixer_input.shape[1] * lax.axis_size("tp")
    sums_a, squares_a = row_moments(mixer_input)
    sums_b, squares_b = row_moments(expert_input)
    sums_a, squares_a, sums_b, squares_b = lax.psum((sums_a, squares_a, sums_b, squares_b), "tp")
    stats_a = jnp.stack([sums_a, squares_a], axis=1)
    normed_b = normalize(expert_input, sums_b, squares_b, expert_gain, width).astype(jnp.bfloat16)
    flat_real = pole_real.reshape(-1)
    flat_imag = pole_imag.reshape(-1)
    denom = flat_real * flat_real + flat_imag * flat_imag
    pole = jnp.stack([flat_real, flat_imag, flat_real / denom, flat_imag / denom])
    mixed = mix(
        mixer_input,
        stats_a,
        mixer_gain[None, :],
        time_step,
        pole,
        input_real.reshape(-1, input_real.shape[2]),
        input_imag.reshape(-1, input_imag.shape[2]),
        read_real.reshape(-1, read_real.shape[2]),
        read_imag.reshape(-1, read_imag.shape[2]),
        width,
    )
    piece = lax.all_gather(mixed, "tp", axis=1, tiled=True)
    value_sum = jnp.dot(piece, out_value, preferred_element_type=jnp.float32)
    gate_sum = jnp.dot(piece, out_gate, preferred_element_type=jnp.float32)
    mixer_output = (value_sum * jax.nn.sigmoid(gate_sum)).astype(jnp.bfloat16)
    tokens_dev, top_count = routes.shape
    expert_count = lax.axis_size("ep")
    capacity = 2 * top_count * tokens_dev // expert_count
    flat_routes = routes.reshape(-1)
    onehot = (flat_routes[:, None] == jnp.arange(expert_count, dtype=jnp.int32)[None, :]).astype(
        jnp.int32
    )
    earlier_hits = jnp.cumsum(onehot, axis=0) - onehot
    position = jnp.sum(earlier_hits * onehot, axis=1)
    slot_index = (flat_routes * capacity + position).reshape(tokens_dev, top_count)
    slots = jnp.arange(expert_count * capacity, dtype=jnp.int32)
    named = slot_index[:, :, None] == slots[None, None, :]
    gate_weight = expert_gate[0]
    up_weight = expert_up[0]
    down_weight = expert_down[0]
    full_rows = lax.all_gather(normed_b, "tp", axis=1, tiled=True)
    chosen = jnp.any(named, axis=1).astype(jnp.bfloat16)
    outgoing = lax.dot_general(
        chosen, full_rows, (((0,), (0,)), ((), ())), preferred_element_type=jnp.float32
    ).astype(jnp.bfloat16)
    arrived = lax.all_to_all(outgoing, "ep", split_axis=0, concat_axis=0, tiled=True)
    gate_val = jnp.dot(arrived, gate_weight, preferred_element_type=jnp.float32)
    up_val = jnp.dot(arrived, up_weight, preferred_element_type=jnp.float32)
    hidden = (jax.nn.silu(gate_val) * up_val).astype(jnp.bfloat16)
    summed = lax.psum_scatter(
        lax.dot_general(
            down_weight, hidden, (((0,), (1,)), ((), ())), preferred_element_type=jnp.float32
        ).astype(jnp.bfloat16),
        "tp",
        scatter_dimension=0,
        tiled=True,
    )
    returned = lax.all_to_all(summed, "ep", split_axis=1, concat_axis=1, tiled=True)
    share = jnp.sum(jnp.where(named, route_weight[:, :, None], 0.0), axis=1)
    share_high = share.astype(jnp.bfloat16)
    share_low = (share - share_high.astype(jnp.float32)).astype(jnp.bfloat16)
    expert_output = (nt(share_high, returned) + nt(share_low, returned)).astype(jnp.bfloat16)
    return (mixer_output, expert_output)


def solution(mesh):
    return jax.shard_map(
        shards,
        mesh=mesh,
        in_specs=(
            P("ep", "tp"),
            P("tp"),
            P("ep", "tp"),
            P("tp", None),
            P("tp", None),
            P("tp", None, None),
            P("tp", None, None),
            P("tp", None, None),
            P("tp", None, None),
            P(None, "tp"),
            P(None, "tp"),
            P("ep", "tp"),
            P("tp"),
            P("ep", None),
            P("ep", None),
            P("ep", None, "tp"),
            P("ep", None, "tp"),
            P("ep", "tp", None),
        ),
        out_specs=(P("ep", "tp"), P("ep", "tp")),
        check_vma=False,
    )
```

```python
import functools
import jax
import jax.numpy as jnp
from jax import lax
from jax.experimental import pallas as pl
from jax.experimental.pallas import tpu as pltpu
from jax.sharding import PartitionSpec as P

norm_eps = 1e-05
highest = lax.Precision.HIGHEST
CHUNKS = 8
TILE = 256


def sin_cos(angle):
    turns = jnp.round(angle * 0.6366197723675814)
    left = angle - turns * 1.5703125
    left = left - turns * 4.83751296997e-4
    left = left - turns * 7.549789948768648e-8
    sq = left * left
    sine = ((-1.9515295891e-4 * sq + 8.3321608736e-3) * sq - 1.6666654611e-1) * sq * left + left
    cosine = (
        ((2.443315711809948e-5 * sq - 1.388731625493765e-3) * sq + 4.166664568298827e-2) * sq * sq
        - 0.5 * sq
        + 1.0
    )
    quadrant = turns.astype(jnp.int32)
    odd = (quadrant & 1) == 1
    sin_out = jnp.where(odd, cosine, sine)
    cos_out = jnp.where(odd, sine, cosine)
    sin_out = jnp.where((quadrant & 2) == 2, -sin_out, sin_out)
    cos_out = jnp.where(((quadrant + 1) & 2) == 2, -cos_out, cos_out)
    return sin_out, cos_out


def nt(left, right, **kw):
    return lax.dot_general(
        left, right, (((1,), (1,)), ((), ())), preferred_element_type=jnp.float32, **kw
    )


def spread(table, row_div, lane_div):
    rows, width = table.shape
    lanes = width * (rows // row_div)
    src = lax.broadcasted_iota(jnp.int32, (width, lanes), 0)
    dst = lax.broadcasted_iota(jnp.int32, (width, lanes), 1)
    pick = (src == dst % width).astype(jnp.bfloat16)
    wide = jnp.dot(table.astype(jnp.bfloat16), pick, preferred_element_type=jnp.float32)
    row = lax.broadcasted_iota(jnp.int32, (rows, lanes), 0) // row_div
    lane = lax.broadcasted_iota(jnp.int32, (rows, lanes), 1) // lane_div
    return jnp.where(row == lane, wide, 0.0).astype(jnp.bfloat16)


def mixer_kernel(
    width,
    rows_ref,
    stats_ref,
    gain_ref,
    step_ref,
    pole_ref,
    in_re_ref,
    in_im_ref,
    rd_re_ref,
    rd_im_ref,
    out_ref,
    a_re,
    a_im,
    u_re,
    u_im,
    sums,
    enter,
    mixed_ref,
    mine_ref,
    slots_ref,
    send_sems,
    recv_sems,
):
    count = slots_ref.shape[0]
    me = lax.axis_index("ep")
    barrier = pltpu.get_barrier_semaphore()
    for k in range(1, count):
        pl.semaphore_signal(
            barrier,
            inc=1,
            device_id={"ep": lax.rem(me + k, count)},
            device_id_type=pl.DeviceIdType.MESH,
        )

    positions, channels = rows_ref.shape
    groups = step_ref.shape[1]
    flat = a_re.shape[1]
    states = flat // groups
    group_ch = channels // groups
    tiles = flat // TILE
    per_tile = TILE // states
    tile_ch = per_tile * group_ch
    steps = positions // CHUNKS

    average = stats_ref[:, 0:1] / width
    variance = stats_ref[:, 1:2] / width - average * average
    normed = (rows_ref[...].astype(jnp.float32) - average) * lax.rsqrt(variance + norm_eps)
    normed = (normed * gain_ref[...]).astype(jnp.bfloat16)
    to_row = lax.broadcasted_iota(jnp.int32, (positions, positions), 0)
    from_row = lax.broadcasted_iota(jnp.int32, (positions, positions), 1)
    order = from_row == (to_row % CHUNKS) * steps + to_row // CHUNKS
    order16 = order.astype(jnp.bfloat16)
    normed = jnp.dot(order16, normed, preferred_element_type=jnp.float32).astype(jnp.bfloat16)
    step = jnp.dot(
        order.astype(jnp.float32), step_ref[...], precision=highest,
        preferred_element_type=jnp.float32,
    )

    for tile in range(tiles):
        lanes = slice(tile * TILE, (tile + 1) * TILE)
        source = lax.broadcasted_iota(jnp.int32, (groups, TILE), 0)
        owner = lax.broadcasted_iota(jnp.int32, (groups, TILE), 1) // states + tile * per_tile
        a_re[:, lanes] = jnp.dot(
            step, (source == owner).astype(jnp.float32), precision=highest,
            preferred_element_type=jnp.float32,
        )
        piece = normed[:, tile * tile_ch : (tile + 1) * tile_ch]
        u_re[:, lanes] = nt(piece, spread(in_re_ref[lanes, :], states, group_ch))
        u_im[:, lanes] = nt(piece, spread(in_im_ref[lanes, :], states, group_ch))
        p_re, p_im = pole_ref[0:1, lanes], pole_ref[1:2, lanes]
        d_re, d_im = pole_ref[2:3, lanes], pole_ref[3:4, lanes]

        def first(s, carried, lanes=lanes, p_re=p_re, p_im=p_im, d_re=d_re, d_im=d_im):
            c_re, c_im, s_re, s_im = carried
            here = pl.ds(pl.multiple_of(s * CHUNKS, CHUNKS), CHUNKS)
            delta = a_re[here, lanes]
            magnitude = jnp.exp(p_re * delta)
            sine, cosine = sin_cos(p_im * delta)
            ab_re = magnitude * cosine
            ab_im = magnitude * sine
            numer = ab_re - 1.0
            k_re = numer * d_re + ab_im * d_im
            k_im = ab_im * d_re - numer * d_im
            v_re, v_im = u_re[here, lanes], u_im[here, lanes]
            w_re = k_re * v_re - k_im * v_im
            w_im = k_re * v_im + k_im * v_re
            a_re[here, lanes] = ab_re
            a_im[here, lanes] = ab_im
            u_re[here, lanes] = w_re
            u_im[here, lanes] = w_im
            return (
                ab_re * c_re - ab_im * c_im,
                ab_re * c_im + ab_im * c_re,
                ab_re * s_re - ab_im * s_im + w_re,
                ab_re * s_im + ab_im * s_re + w_im,
            )

        zero = jnp.zeros((CHUNKS, TILE), jnp.float32)
        found = lax.fori_loop(0, steps, first, (zero + 1.0, zero, zero, zero), unroll=4)
        for index, part in enumerate(found):
            sums[index, :, lanes] = part

    def chunk(index, c):
        return sums[index, c : c + 1, :]

    c_re, c_im, s_re, s_im = (chunk(index, 0) for index in range(4))
    for c in range(1, CHUNKS):
        b_re, b_im = chunk(0, c), chunk(1, c)
        c_re, c_im = b_re * c_re - b_im * c_im, b_re * c_im + b_im * c_re
        s_re, s_im = (
            b_re * s_re - b_im * s_im + chunk(2, c),
            b_re * s_im + b_im * s_re + chunk(3, c),
        )
    mine_ref[0:1, :] = c_re
    mine_ref[1:2, :] = c_im
    mine_ref[2:3, :] = s_re
    mine_ref[3:4, :] = s_im

    pl.semaphore_wait(barrier, count - 1)
    copies = []
    for k in range(1, count):
        copy = pltpu.make_async_remote_copy(
            src_ref=mine_ref,
            dst_ref=slots_ref.at[k],
            send_sem=send_sems.at[k],
            recv_sem=recv_sems.at[k],
            device_id={"ep": lax.rem(me + k, count)},
            device_id_type=pl.DeviceIdType.MESH,
        )
        copy.start()
        copies.append(copy)
    read_re = [
        spread(rd_re_ref[t * tile_ch : (t + 1) * tile_ch, :], group_ch, states)
        for t in range(tiles)
    ]
    read_im = [
        spread(rd_im_ref[t * tile_ch : (t + 1) * tile_ch, :], group_ch, states)
        for t in range(tiles)
    ]
    for copy in copies:
        copy.wait()

    def fold(position, carried):
        h_re, h_im = carried
        slot = me - position
        b_re, b_im = slots_ref[slot, 0:1, :], slots_ref[slot, 1:2, :]
        return (
            b_re * h_re - b_im * h_im + slots_ref[slot, 2:3, :],
            b_re * h_im + b_im * h_re + slots_ref[slot, 3:4, :],
        )

    blank = jnp.zeros((1, flat), jnp.float32)
    h_re, h_im = lax.fori_loop(0, me, fold, (blank, blank))
    for c in range(CHUNKS):
        enter[0, c : c + 1, :] = h_re
        enter[1, c : c + 1, :] = h_im
        b_re, b_im = chunk(0, c), chunk(1, c)
        h_re, h_im = (
            b_re * h_re - b_im * h_im + chunk(2, c),
            b_re * h_im + b_im * h_re + chunk(3, c),
        )

    for tile in range(tiles):
        lanes = slice(tile * TILE, (tile + 1) * TILE)

        def second(s, carried, lanes=lanes):
            s_re, s_im = carried
            here = pl.ds(pl.multiple_of(s * CHUNKS, CHUNKS), CHUNKS)
            ab_re, ab_im = a_re[here, lanes], a_im[here, lanes]
            n_re = ab_re * s_re - ab_im * s_im + u_re[here, lanes]
            n_im = ab_re * s_im + ab_im * s_re + u_im[here, lanes]
            u_re[here, lanes] = n_re
            u_im[here, lanes] = n_im
            return n_re, n_im

        lax.fori_loop(0, steps, second, (enter[0, :, lanes], enter[1, :, lanes]), unroll=8)
        response = nt(u_re[:, lanes].astype(jnp.bfloat16), read_re[tile]) - nt(
            u_im[:, lanes].astype(jnp.bfloat16), read_im[tile]
        )
        mixed_ref[:, tile * tile_ch : (tile + 1) * tile_ch] = jax.nn.gelu(response).astype(
            jnp.bfloat16
        )
    back = (to_row == (from_row % CHUNKS) * steps + from_row // CHUNKS).astype(jnp.bfloat16)
    out_ref[...] = jnp.dot(
        back, mixed_ref[...], preferred_element_type=jnp.float32
    ).astype(jnp.bfloat16)


def mix(rows, stats, gain, step, pole, in_re, in_im, rd_re, rd_im, width):
    positions, channels = rows.shape
    flat = pole.shape[1]
    count = lax.axis_size("ep")
    f32 = jnp.float32
    return pl.pallas_call(
        functools.partial(mixer_kernel, width),
        out_shape=jax.ShapeDtypeStruct((positions, channels), jnp.bfloat16),
        in_specs=[pl.BlockSpec(memory_space=pltpu.VMEM)] * 9,
        out_specs=pl.BlockSpec(memory_space=pltpu.VMEM),
        scratch_shapes=[
            pltpu.VMEM((positions, flat), f32),
            pltpu.VMEM((positions, flat), f32),
            pltpu.VMEM((positions, flat), f32),
            pltpu.VMEM((positions, flat), f32),
            pltpu.VMEM((4, CHUNKS, flat), f32),
            pltpu.VMEM((2, CHUNKS, flat), f32),
            pltpu.VMEM((positions, channels), jnp.bfloat16),
            pltpu.VMEM((4, flat), f32),
            pltpu.VMEM((count, 4, flat), f32),
            pltpu.SemaphoreType.DMA((count,)),
            pltpu.SemaphoreType.DMA((count,)),
        ],
        compiler_params=pltpu.CompilerParams(
            collective_id=0, has_side_effects=True, vmem_limit_bytes=24 * 1024 * 1024
        ),
        cost_estimate=pl.CostEstimate(
            flops=2 * positions * flat * 400, bytes_accessed=4 * positions * flat, transcendentals=0
        ),
    )(rows, stats, gain, step, pole, in_re, in_im, rd_re, rd_im)


def moments_kernel(a_ref, b_ref, out_a_ref, out_b_ref, mine_ref, slots_ref, send_sems, recv_sems):
    count = slots_ref.shape[0]
    me = lax.axis_index("tp")
    barrier = pltpu.get_barrier_semaphore()
    for k in range(1, count):
        pl.semaphore_signal(
            barrier,
            inc=1,
            device_id={"tp": lax.rem(me + k, count)},
            device_id_type=pl.DeviceIdType.MESH,
        )
    split = a_ref.shape[0]
    ones = jnp.ones((8, a_ref.shape[1]), jnp.float32)
    first = lax.broadcasted_iota(jnp.int32, (8, 1), 0) == 0
    for rows_ref, lanes in ((a_ref, slice(0, split)), (b_ref, slice(split, None))):
        wide = rows_ref[...].astype(jnp.float32)
        sums = nt(ones, wide, precision=highest)
        squares = nt(ones, wide * wide, precision=highest)
        mine_ref[:, lanes] = jnp.where(first, sums, squares)
    pl.semaphore_wait(barrier, count - 1)
    copies = []
    for k in range(1, count):
        copy = pltpu.make_async_remote_copy(
            src_ref=mine_ref,
            dst_ref=slots_ref.at[k],
            send_sem=send_sems.at[k],
            recv_sem=recv_sems.at[k],
            device_id={"tp": lax.rem(me + k, count)},
            device_id_type=pl.DeviceIdType.MESH,
        )
        copy.start()
        copies.append(copy)
    total = mine_ref[...]
    for k, copy in enumerate(copies):
        copy.wait()
        total = total + slots_ref[k + 1]
    turned = total.T
    out_a_ref[...] = turned[:split, :]
    out_b_ref[...] = turned[split:, :]


def moments(rows_a, rows_b):
    count = lax.axis_size("tp")
    size = rows_a.shape[0] + rows_b.shape[0]
    f32 = jnp.float32
    return pl.pallas_call(
        moments_kernel,
        out_shape=[
            jax.ShapeDtypeStruct((rows_a.shape[0], 8), f32),
            jax.ShapeDtypeStruct((rows_b.shape[0], 8), f32),
        ],
        in_specs=[pl.BlockSpec(memory_space=pltpu.VMEM)] * 2,
        out_specs=[pl.BlockSpec(memory_space=pltpu.VMEM)] * 2,
        scratch_shapes=[
            pltpu.VMEM((8, size), f32),
            pltpu.VMEM((count, 8, size), f32),
            pltpu.SemaphoreType.DMA((count,)),
            pltpu.SemaphoreType.DMA((count,)),
        ],
        compiler_params=pltpu.CompilerParams(
            collective_id=1, has_side_effects=True, vmem_limit_bytes=16 * 1024 * 1024
        ),
    )(rows_a, rows_b)


def normalize(rows, sums, squares, gain, width):
    average = sums / width
    variance = squares / width - average * average
    wide = rows.astype(jnp.float32)
    return (wide - average[:, None]) * lax.rsqrt(variance[:, None] + norm_eps) * gain[None, :]


def shards(
    mixer_input,
    mixer_gain,
    time_step,
    pole_real,
    pole_imag,
    input_real,
    input_imag,
    read_real,
    read_imag,
    out_value,
    out_gate,
    expert_input,
    expert_gain,
    routes,
    route_weight,
    expert_gate,
    expert_up,
    expert_down,
):
    width = mixer_input.shape[1] * lax.axis_size("tp")
    stats_a, stats_b = moments(mixer_input, expert_input)
    sums_b, squares_b = stats_b[:, 0], stats_b[:, 1]
    normed_b = normalize(expert_input, sums_b, squares_b, expert_gain, width).astype(jnp.bfloat16)
    tokens_dev, top_count = routes.shape
    expert_count = lax.axis_size("ep")
    capacity = 2 * top_count * tokens_dev // expert_count
    flat_routes = routes.reshape(-1)
    onehot = (flat_routes[:, None] == jnp.arange(expert_count, dtype=jnp.int32)[None, :]).astype(
        jnp.int32
    )
    earlier_hits = jnp.cumsum(onehot, axis=0) - onehot
    position = jnp.sum(earlier_hits * onehot, axis=1)
    slot_index = (flat_routes * capacity + position).reshape(tokens_dev, top_count)
    slots = jnp.arange(expert_count * capacity, dtype=jnp.int32)
    named = slot_index[:, :, None] == slots[None, None, :]
    gate_weight = expert_gate[0]
    up_weight = expert_up[0]
    down_weight = expert_down[0]
    chosen = jnp.any(named, axis=1).astype(jnp.bfloat16)
    outgoing = lax.dot_general(
        chosen, normed_b, (((0,), (0,)), ((), ())), preferred_element_type=jnp.float32
    ).astype(jnp.bfloat16)
    arrived = lax.all_to_all(outgoing, "ep", split_axis=0, concat_axis=0, tiled=True)
    flat_real = pole_real.reshape(-1)
    flat_imag = pole_imag.reshape(-1)
    denom = flat_real * flat_real + flat_imag * flat_imag
    pole = jnp.stack([flat_real, flat_imag, flat_real / denom, flat_imag / denom])
    arrived, stats_a = lax.optimization_barrier((arrived, stats_a))
    arrived = lax.all_gather(arrived, "tp", axis=1, tiled=True)
    mixed = mix(
        mixer_input,
        stats_a,
        mixer_gain[None, :],
        time_step,
        pole,
        input_real.reshape(-1, input_real.shape[2]),
        input_imag.reshape(-1, input_imag.shape[2]),
        read_real.reshape(-1, read_real.shape[2]),
        read_imag.reshape(-1, read_imag.shape[2]),
        width,
    )
    arrived, mixed = lax.optimization_barrier((arrived, mixed))
    piece = lax.all_gather(mixed, "tp", axis=1, tiled=True)
    gate_val = jnp.dot(arrived, gate_weight, preferred_element_type=jnp.float32)
    up_val = jnp.dot(arrived, up_weight, preferred_element_type=jnp.float32)
    hidden = (jax.nn.silu(gate_val) * up_val).astype(jnp.bfloat16)
    summed = lax.psum_scatter(
        lax.dot_general(
            down_weight, hidden, (((0,), (1,)), ((), ())), preferred_element_type=jnp.float32
        ).astype(jnp.bfloat16),
        "tp",
        scatter_dimension=0,
        tiled=True,
    )
    value_sum = jnp.dot(piece, out_value, preferred_element_type=jnp.float32)
    gate_sum = jnp.dot(piece, out_gate, preferred_element_type=jnp.float32)
    mixer_output = (value_sum * jax.nn.sigmoid(gate_sum)).astype(jnp.bfloat16)
    returned = lax.all_to_all(summed, "ep", split_axis=1, concat_axis=1, tiled=True)
    share = jnp.sum(jnp.where(named, route_weight[:, :, None], 0.0), axis=1)
    share_high = share.astype(jnp.bfloat16)
    share_low = (share - share_high.astype(jnp.float32)).astype(jnp.bfloat16)
    expert_output = (nt(share_high, returned) + nt(share_low, returned)).astype(jnp.bfloat16)
    return (mixer_output, expert_output)


def solution(mesh):
    return jax.shard_map(
        shards,
        mesh=mesh,
        in_specs=(
            P("ep", "tp"),
            P("tp"),
            P("ep", "tp"),
            P("tp", None),
            P("tp", None),
            P("tp", None, None),
            P("tp", None, None),
            P("tp", None, None),
            P("tp", None, None),
            P(None, "tp"),
            P(None, "tp"),
            P("ep", "tp"),
            P("tp"),
            P("ep", None),
            P("ep", None),
            P("ep", None, "tp"),
            P("ep", None, "tp"),
            P("ep", "tp", None),
        ),
        out_specs=(P("ep", "tp"), P("ep", "tp")),
        check_vma=False,
    )
```

```python
import functools
import jax
import jax.numpy as jnp
from jax import lax
from jax.experimental import pallas as pl
from jax.experimental.pallas import tpu as pltpu
from jax.sharding import PartitionSpec as P

norm_eps = 1e-05
highest = lax.Precision.HIGHEST
CHUNKS = 8
TILE = 256


def sin_cos(angle):
    turns = jnp.round(angle * 0.6366197723675814)
    left = angle - turns * 1.5703125
    left = left - turns * 4.83751296997e-4
    left = left - turns * 7.549789948768648e-8
    sq = left * left
    sine = ((-1.9515295891e-4 * sq + 8.3321608736e-3) * sq - 1.6666654611e-1) * sq * left + left
    cosine = (
        ((2.443315711809948e-5 * sq - 1.388731625493765e-3) * sq + 4.166664568298827e-2) * sq * sq
        - 0.5 * sq
        + 1.0
    )
    quadrant = turns.astype(jnp.int32)
    odd = (quadrant & 1) == 1
    sin_out = jnp.where(odd, cosine, sine)
    cos_out = jnp.where(odd, sine, cosine)
    sin_out = jnp.where((quadrant & 2) == 2, -sin_out, sin_out)
    cos_out = jnp.where(((quadrant + 1) & 2) == 2, -cos_out, cos_out)
    return sin_out, cos_out


def nt(left, right, **kw):
    return lax.dot_general(
        left, right, (((1,), (1,)), ((), ())), preferred_element_type=jnp.float32, **kw
    )


def spread(table, row_div, lane_div):
    rows, width = table.shape
    lanes = width * (rows // row_div)
    src = lax.broadcasted_iota(jnp.int32, (width, lanes), 0)
    dst = lax.broadcasted_iota(jnp.int32, (width, lanes), 1)
    pick = (src == dst % width).astype(jnp.bfloat16)
    wide = jnp.dot(table.astype(jnp.bfloat16), pick, preferred_element_type=jnp.float32)
    row = lax.broadcasted_iota(jnp.int32, (rows, lanes), 0) // row_div
    lane = lax.broadcasted_iota(jnp.int32, (rows, lanes), 1) // lane_div
    return jnp.where(row == lane, wide, 0.0).astype(jnp.bfloat16)


def mixer_kernel(
    width,
    rows_ref,
    stats_ref,
    gain_ref,
    step_ref,
    pole_ref,
    in_re_ref,
    in_im_ref,
    rd_re_ref,
    rd_im_ref,
    out_ref,
    a_re,
    a_im,
    u_re,
    u_im,
    sums,
    enter,
    mixed_ref,
    mine_ref,
    slots_ref,
    send_sems,
    recv_sems,
):
    count = slots_ref.shape[0]
    me = lax.axis_index("ep")
    barrier = pltpu.get_barrier_semaphore()
    for k in range(1, count):
        pl.semaphore_signal(
            barrier,
            inc=1,
            device_id={"ep": lax.rem(me + k, count)},
            device_id_type=pl.DeviceIdType.MESH,
        )

    positions, channels = rows_ref.shape
    groups = step_ref.shape[1]
    flat = a_re.shape[1]
    states = flat // groups
    group_ch = channels // groups
    tiles = flat // TILE
    per_tile = TILE // states
    tile_ch = per_tile * group_ch
    steps = positions // CHUNKS

    average = stats_ref[:, 0:1] / width
    variance = stats_ref[:, 1:2] / width - average * average
    normed = (rows_ref[...].astype(jnp.float32) - average) * lax.rsqrt(variance + norm_eps)
    normed = (normed * gain_ref[...]).astype(jnp.bfloat16)
    to_row = lax.broadcasted_iota(jnp.int32, (positions, positions), 0)
    from_row = lax.broadcasted_iota(jnp.int32, (positions, positions), 1)
    order = from_row == (to_row % CHUNKS) * steps + to_row // CHUNKS
    order16 = order.astype(jnp.bfloat16)
    normed = jnp.dot(order16, normed, preferred_element_type=jnp.float32).astype(jnp.bfloat16)
    step = jnp.dot(
        order.astype(jnp.float32), step_ref[...], precision=highest,
        preferred_element_type=jnp.float32,
    )

    for tile in range(tiles):
        lanes = slice(tile * TILE, (tile + 1) * TILE)
        source = lax.broadcasted_iota(jnp.int32, (groups, TILE), 0)
        owner = lax.broadcasted_iota(jnp.int32, (groups, TILE), 1) // states + tile * per_tile
        a_re[:, lanes] = jnp.dot(
            step, (source == owner).astype(jnp.float32), precision=highest,
            preferred_element_type=jnp.float32,
        )
        piece = normed[:, tile * tile_ch : (tile + 1) * tile_ch]
        u_re[:, lanes] = nt(piece, spread(in_re_ref[lanes, :], states, group_ch))
        u_im[:, lanes] = nt(piece, spread(in_im_ref[lanes, :], states, group_ch))
        p_re, p_im = pole_ref[0:1, lanes], pole_ref[1:2, lanes]
        d_re, d_im = pole_ref[2:3, lanes], pole_ref[3:4, lanes]

        def first(s, carried, lanes=lanes, p_re=p_re, p_im=p_im, d_re=d_re, d_im=d_im):
            c_re, c_im, s_re, s_im = carried
            here = pl.ds(pl.multiple_of(s * CHUNKS, CHUNKS), CHUNKS)
            delta = a_re[here, lanes]
            magnitude = jnp.exp(p_re * delta)
            sine, cosine = sin_cos(p_im * delta)
            ab_re = magnitude * cosine
            ab_im = magnitude * sine
            numer = ab_re - 1.0
            k_re = numer * d_re + ab_im * d_im
            k_im = ab_im * d_re - numer * d_im
            v_re, v_im = u_re[here, lanes], u_im[here, lanes]
            w_re = k_re * v_re - k_im * v_im
            w_im = k_re * v_im + k_im * v_re
            a_re[here, lanes] = ab_re
            a_im[here, lanes] = ab_im
            u_re[here, lanes] = w_re
            u_im[here, lanes] = w_im
            return (
                ab_re * c_re - ab_im * c_im,
                ab_re * c_im + ab_im * c_re,
                ab_re * s_re - ab_im * s_im + w_re,
                ab_re * s_im + ab_im * s_re + w_im,
            )

        zero = jnp.zeros((CHUNKS, TILE), jnp.float32)
        found = lax.fori_loop(0, steps, first, (zero + 1.0, zero, zero, zero), unroll=4)
        for index, part in enumerate(found):
            sums[index, :, lanes] = part

    def chunk(index, c):
        return sums[index, c : c + 1, :]

    c_re, c_im, s_re, s_im = (chunk(index, 0) for index in range(4))
    for c in range(1, CHUNKS):
        b_re, b_im = chunk(0, c), chunk(1, c)
        c_re, c_im = b_re * c_re - b_im * c_im, b_re * c_im + b_im * c_re
        s_re, s_im = (
            b_re * s_re - b_im * s_im + chunk(2, c),
            b_re * s_im + b_im * s_re + chunk(3, c),
        )
    mine_ref[0:1, :] = c_re
    mine_ref[1:2, :] = c_im
    mine_ref[2:3, :] = s_re
    mine_ref[3:4, :] = s_im

    pl.semaphore_wait(barrier, count - 1)
    copies = []
    for k in range(1, count):
        copy = pltpu.make_async_remote_copy(
            src_ref=mine_ref,
            dst_ref=slots_ref.at[k],
            send_sem=send_sems.at[k],
            recv_sem=recv_sems.at[k],
            device_id={"ep": lax.rem(me + k, count)},
            device_id_type=pl.DeviceIdType.MESH,
        )
        copy.start()
        copies.append(copy)
    read_re = [
        spread(rd_re_ref[t * tile_ch : (t + 1) * tile_ch, :], group_ch, states)
        for t in range(tiles)
    ]
    read_im = [
        spread(rd_im_ref[t * tile_ch : (t + 1) * tile_ch, :], group_ch, states)
        for t in range(tiles)
    ]
    for copy in copies:
        copy.wait()

    def fold(position, carried):
        h_re, h_im = carried
        slot = me - position
        b_re, b_im = slots_ref[slot, 0:1, :], slots_ref[slot, 1:2, :]
        return (
            b_re * h_re - b_im * h_im + slots_ref[slot, 2:3, :],
            b_re * h_im + b_im * h_re + slots_ref[slot, 3:4, :],
        )

    blank = jnp.zeros((1, flat), jnp.float32)
    h_re, h_im = lax.fori_loop(0, me, fold, (blank, blank))
    for c in range(CHUNKS):
        enter[0, c : c + 1, :] = h_re
        enter[1, c : c + 1, :] = h_im
        b_re, b_im = chunk(0, c), chunk(1, c)
        h_re, h_im = (
            b_re * h_re - b_im * h_im + chunk(2, c),
            b_re * h_im + b_im * h_re + chunk(3, c),
        )

    for tile in range(tiles):
        lanes = slice(tile * TILE, (tile + 1) * TILE)

        def second(s, carried, lanes=lanes):
            s_re, s_im = carried
            here = pl.ds(pl.multiple_of(s * CHUNKS, CHUNKS), CHUNKS)
            ab_re, ab_im = a_re[here, lanes], a_im[here, lanes]
            n_re = ab_re * s_re - ab_im * s_im + u_re[here, lanes]
            n_im = ab_re * s_im + ab_im * s_re + u_im[here, lanes]
            u_re[here, lanes] = n_re
            u_im[here, lanes] = n_im
            return n_re, n_im

        lax.fori_loop(0, steps, second, (enter[0, :, lanes], enter[1, :, lanes]), unroll=8)
        response = nt(u_re[:, lanes].astype(jnp.bfloat16), read_re[tile]) - nt(
            u_im[:, lanes].astype(jnp.bfloat16), read_im[tile]
        )
        mixed_ref[:, tile * tile_ch : (tile + 1) * tile_ch] = jax.nn.gelu(response).astype(
            jnp.bfloat16
        )
    back = (to_row == (from_row % CHUNKS) * steps + from_row // CHUNKS).astype(jnp.bfloat16)
    out_ref[...] = jnp.dot(
        back, mixed_ref[...], preferred_element_type=jnp.float32
    ).astype(jnp.bfloat16)


def mix(rows, stats, gain, step, pole, in_re, in_im, rd_re, rd_im, width):
    positions, channels = rows.shape
    flat = pole.shape[1]
    count = lax.axis_size("ep")
    f32 = jnp.float32
    return pl.pallas_call(
        functools.partial(mixer_kernel, width),
        out_shape=jax.ShapeDtypeStruct((positions, channels), jnp.bfloat16),
        in_specs=[pl.BlockSpec(memory_space=pltpu.VMEM)] * 9,
        out_specs=pl.BlockSpec(memory_space=pltpu.VMEM),
        scratch_shapes=[
            pltpu.VMEM((positions, flat), f32),
            pltpu.VMEM((positions, flat), f32),
            pltpu.VMEM((positions, flat), f32),
            pltpu.VMEM((positions, flat), f32),
            pltpu.VMEM((4, CHUNKS, flat), f32),
            pltpu.VMEM((2, CHUNKS, flat), f32),
            pltpu.VMEM((positions, channels), jnp.bfloat16),
            pltpu.VMEM((4, flat), f32),
            pltpu.VMEM((count, 4, flat), f32),
            pltpu.SemaphoreType.DMA((count,)),
            pltpu.SemaphoreType.DMA((count,)),
        ],
        compiler_params=pltpu.CompilerParams(
            collective_id=0, has_side_effects=True, vmem_limit_bytes=24 * 1024 * 1024
        ),
        cost_estimate=pl.CostEstimate(
            flops=2 * positions * flat * 400, bytes_accessed=4 * positions * flat, transcendentals=0
        ),
    )(rows, stats, gain, step, pole, in_re, in_im, rd_re, rd_im)


def moments_kernel(a_ref, b_ref, out_a_ref, out_b_ref, mine_ref, slots_ref, send_sems, recv_sems):
    count = slots_ref.shape[0]
    me = lax.axis_index("tp")
    barrier = pltpu.get_barrier_semaphore()
    for k in range(1, count):
        pl.semaphore_signal(
            barrier,
            inc=1,
            device_id={"tp": lax.rem(me + k, count)},
            device_id_type=pl.DeviceIdType.MESH,
        )
    split = a_ref.shape[0]
    ones = jnp.ones((8, a_ref.shape[1]), jnp.float32)
    first = lax.broadcasted_iota(jnp.int32, (8, 1), 0) == 0
    for rows_ref, lanes in ((a_ref, slice(0, split)), (b_ref, slice(split, None))):
        wide = rows_ref[...].astype(jnp.float32)
        sums = nt(ones, wide, precision=highest)
        squares = nt(ones, wide * wide, precision=highest)
        mine_ref[:, lanes] = jnp.where(first, sums, squares)
    pl.semaphore_wait(barrier, count - 1)
    copies = []
    for k in range(1, count):
        copy = pltpu.make_async_remote_copy(
            src_ref=mine_ref,
            dst_ref=slots_ref.at[k],
            send_sem=send_sems.at[k],
            recv_sem=recv_sems.at[k],
            device_id={"tp": lax.rem(me + k, count)},
            device_id_type=pl.DeviceIdType.MESH,
        )
        copy.start()
        copies.append(copy)
    total = mine_ref[...]
    for k, copy in enumerate(copies):
        copy.wait()
        total = total + slots_ref[k + 1]
    turned = total.T
    out_a_ref[...] = turned[:split, :]
    out_b_ref[...] = turned[split:, :]


def moments(rows_a, rows_b):
    count = lax.axis_size("tp")
    size = rows_a.shape[0] + rows_b.shape[0]
    f32 = jnp.float32
    return pl.pallas_call(
        moments_kernel,
        out_shape=[
            jax.ShapeDtypeStruct((rows_a.shape[0], 8), f32),
            jax.ShapeDtypeStruct((rows_b.shape[0], 8), f32),
        ],
        in_specs=[pl.BlockSpec(memory_space=pltpu.VMEM)] * 2,
        out_specs=[pl.BlockSpec(memory_space=pltpu.VMEM)] * 2,
        scratch_shapes=[
            pltpu.VMEM((8, size), f32),
            pltpu.VMEM((count, 8, size), f32),
            pltpu.SemaphoreType.DMA((count,)),
            pltpu.SemaphoreType.DMA((count,)),
        ],
        compiler_params=pltpu.CompilerParams(
            collective_id=1, has_side_effects=True, vmem_limit_bytes=16 * 1024 * 1024
        ),
    )(rows_a, rows_b)


def normalize(rows, sums, squares, gain, width):
    average = sums / width
    variance = squares / width - average * average
    wide = rows.astype(jnp.float32)
    return (wide - average[:, None]) * lax.rsqrt(variance[:, None] + norm_eps) * gain[None, :]


def scatter_sum(partial):
    count = lax.axis_size("tp")
    if count != 4:
        return lax.psum_scatter(partial, "tp", scatter_dimension=0, tiled=True)
    blocks = partial.reshape(count, partial.shape[0] // count, partial.shape[1])
    me = lax.axis_index("tp")
    core, far = me % 2, 2 - me // 2 * 2

    def block(index):
        return lax.dynamic_index_in_dim(blocks, index, 0, keepdims=False)

    cores = [(0, 1), (1, 0), (2, 3), (3, 2)]
    chips = [(0, 2), (2, 0), (1, 3), (3, 1)]
    got_far = lax.ppermute(block(far + 1 - core), "tp", cores)
    got_near = lax.ppermute(block(2 - far + 1 - core), "tp", cores)
    half = block(far + core).astype(jnp.float32) + got_far.astype(jnp.float32)
    across = lax.ppermute(half.astype(jnp.bfloat16), "tp", chips)
    near = block(me).astype(jnp.float32) + got_near.astype(jnp.float32)
    return (near + across.astype(jnp.float32)).astype(jnp.bfloat16)


def shards(
    mixer_input,
    mixer_gain,
    time_step,
    pole_real,
    pole_imag,
    input_real,
    input_imag,
    read_real,
    read_imag,
    out_value,
    out_gate,
    expert_input,
    expert_gain,
    routes,
    route_weight,
    expert_gate,
    expert_up,
    expert_down,
):
    width = mixer_input.shape[1] * lax.axis_size("tp")
    stats_a, stats_b = moments(mixer_input, expert_input)
    sums_b, squares_b = stats_b[:, 0], stats_b[:, 1]
    normed_b = normalize(expert_input, sums_b, squares_b, expert_gain, width).astype(jnp.bfloat16)
    tokens_dev, top_count = routes.shape
    expert_count = lax.axis_size("ep")
    capacity = 2 * top_count * tokens_dev // expert_count
    flat_routes = routes.reshape(-1)
    onehot = (flat_routes[:, None] == jnp.arange(expert_count, dtype=jnp.int32)[None, :]).astype(
        jnp.int32
    )
    earlier_hits = jnp.cumsum(onehot, axis=0) - onehot
    position = jnp.sum(earlier_hits * onehot, axis=1)
    slot_index = (flat_routes * capacity + position).reshape(tokens_dev, top_count)
    slots = jnp.arange(expert_count * capacity, dtype=jnp.int32)
    named = slot_index[:, :, None] == slots[None, None, :]
    gate_weight = expert_gate[0]
    up_weight = expert_up[0]
    down_weight = expert_down[0]
    chosen = jnp.any(named, axis=1).astype(jnp.bfloat16)
    outgoing = lax.dot_general(
        chosen, normed_b, (((0,), (0,)), ((), ())), preferred_element_type=jnp.float32
    ).astype(jnp.bfloat16)
    arrived = lax.all_to_all(outgoing, "ep", split_axis=0, concat_axis=0, tiled=True)
    flat_real = pole_real.reshape(-1)
    flat_imag = pole_imag.reshape(-1)
    denom = flat_real * flat_real + flat_imag * flat_imag
    pole = jnp.stack([flat_real, flat_imag, flat_real / denom, flat_imag / denom])
    arrived, stats_a = lax.optimization_barrier((arrived, stats_a))
    arrived = lax.all_gather(arrived, "tp", axis=1, tiled=True)
    mixed = mix(
        mixer_input,
        stats_a,
        mixer_gain[None, :],
        time_step,
        pole,
        input_real.reshape(-1, input_real.shape[2]),
        input_imag.reshape(-1, input_imag.shape[2]),
        read_real.reshape(-1, read_real.shape[2]),
        read_imag.reshape(-1, read_imag.shape[2]),
        width,
    )
    arrived, mixed = lax.optimization_barrier((arrived, mixed))
    piece = lax.all_gather(mixed, "tp", axis=1, tiled=True)
    gate_val = jnp.dot(arrived, gate_weight, preferred_element_type=jnp.float32)
    up_val = jnp.dot(arrived, up_weight, preferred_element_type=jnp.float32)
    hidden = (jax.nn.silu(gate_val) * up_val).astype(jnp.bfloat16)
    hidden, piece = lax.optimization_barrier((hidden, piece))
    partial = lax.dot_general(
        down_weight, hidden, (((0,), (1,)), ((), ())), preferred_element_type=jnp.float32
    ).astype(jnp.bfloat16)
    summed = scatter_sum(partial)
    value_sum = jnp.dot(piece, out_value, preferred_element_type=jnp.float32)
    gate_sum = jnp.dot(piece, out_gate, preferred_element_type=jnp.float32)
    mixer_output = (value_sum * jax.nn.sigmoid(gate_sum)).astype(jnp.bfloat16)
    returned = lax.all_to_all(summed, "ep", split_axis=1, concat_axis=1, tiled=True)
    share = jnp.sum(jnp.where(named, route_weight[:, :, None], 0.0), axis=1)
    share_high = share.astype(jnp.bfloat16)
    share_low = (share - share_high.astype(jnp.float32)).astype(jnp.bfloat16)
    expert_output = (nt(share_high, returned) + nt(share_low, returned)).astype(jnp.bfloat16)
    return (mixer_output, expert_output)


def solution(mesh):
    return jax.shard_map(
        shards,
        mesh=mesh,
        in_specs=(
            P("ep", "tp"),
            P("tp"),
            P("ep", "tp"),
            P("tp", None),
            P("tp", None),
            P("tp", None, None),
            P("tp", None, None),
            P("tp", None, None),
            P("tp", None, None),
            P(None, "tp"),
            P(None, "tp"),
            P("ep", "tp"),
            P("tp"),
            P("ep", None),
            P("ep", None),
            P("ep", None, "tp"),
            P("ep", None, "tp"),
            P("ep", "tp", None),
        ),
        out_specs=(P("ep", "tp"), P("ep", "tp")),
        check_vma=False,
    )
```
